32 devices in a mesh: grp: 2 (over y), sp: 4 (over z), tp: 4 (over x, core).
Axes of the slice: x: 2, y: 2, z: 4, core: 2. Of those that a mesh axis runs over, the one named last changes fastest.
Arguments:
- latents: bfloat16 [2048, 4, 2048], P(('sp', 'tp'), 'grp'), parts along dimension 1, may hold values from -6 to 6
- context: bfloat16 [1024, 4, 2048], P('sp', 'grp'), parts along dimension 1, may hold values from -6 to 6
- condition: float32 [4, 2048], P('grp', 'sp'), parts along dimension 0, may hold values from -6 to 6
- cond_context: float32 [2048], P('sp'), may hold values from -6 to 6
- w_shift: bfloat16 [2048, 2048], P('sp', 'tp'), may hold values from -0.125 to 0.125
- w_scale: bfloat16 [2048, 2048], P('sp', 'tp'), may hold values from -0.125 to 0.125
- w_gate: bfloat16 [2048, 2048], P('sp', 'tp'), may hold values from -0.375 to 0.375
- norm_gain: float32 [2048], replicated, may hold values from 0.1 to 1.9
- w_query: bfloat16 [2048, 1024], P(None, 'tp'), may hold values from -0.375 to 0.375
- w_key: bfloat16 [2048, 512], P(None, 'tp'), may hold values from -0.125 to 0.125
- w_value: bfloat16 [2048, 512], P(None, 'tp'), may hold values from -0.25 to 0.25
- sink_logit: float32 [16], P('tp'), may hold values from 6 to 240
- w_out: bfloat16 [1024, 2048], P('tp'), may hold values from -0.1875 to 0.1875
Outputs:
- refined: bfloat16 [2048, 4, 2048], P(('sp', 'tp'), 'grp'), parts along dimension 1
The draws below stay inside these ranges and needn't reach their ends.
There are 2 independent parts, one for each index of `grp`. The reference program is written for one: setup_inputs(seed, part) draws one part's arguments, and reference() takes and returns one part's arrays. A program takes and returns all parts, laid end to end along the dimension named above; an argument that names none is the same for every part. Nothing has to cross between parts.
All inputs are finite; a program needn't handle non-finite values.
Results may differ from the reference program's by a relative error of at most 0.017.
Values may be sent and summed in bfloat16 or wider, within the bound.
No kernel may reach another device: no remote copies, remote signals or barrier semaphores. Data moves between devices by JAX's collectives and lax.ppermute only.
A program may use at most 128 MiB of HBM per device.

```python
import jax
import jax.numpy as jnp
from jax import lax

D = 2048
N_HEADS = 16
N_KV = 8
HEAD_DIM = 64
WINDOW = 128
GRID_W = 64
CTX = 1024
SAMPLES = 2
TOK_DEV = 512
LATENT = 2048
N_TP = 4


def draw_sink_logit(key, part):
    key_base = jax.random.fold_in(key, 11)
    low_sinks = jax.random.uniform(jax.random.fold_in(key_base, 1), (N_HEADS,), jnp.float32, 6.0, 12.0)
    return low_sinks


def shard_levels(stream_key, shape, shards, low, high):
    def one(axis_at, parts):
        steps = jax.random.uniform(jax.random.fold_in(jax.random.fold_in(stream_key, 6), axis_at), (parts,), jnp.float32, low / len(shards), high / len(shards))
        return jnp.repeat(jnp.exp(steps), shape[axis_at] // parts).reshape((-1,) + (1,) * (len(shape) - axis_at - 1))

    factor_of = one(*shards[0])
    for cut in shards[1:]:
        factor_of = factor_of * one(*cut)
    return factor_of


def normal_values(rng, dims, spread, most, split=(), held_as=jnp.bfloat16):
    level = shard_levels(rng, dims, split, -0.22, 0.18) if split else 1.0
    entries = jax.random.normal(rng, dims, jnp.float32) * spread * level
    return jnp.minimum(jnp.maximum(entries, -most), most).astype(held_as)


def setup_inputs(seed: int = 0, part: int = 0) -> dict:
    streams_of = jax.random.split(jax.random.key(seed), 14)
    part_keys = jax.random.split(jax.random.fold_in(streams_of[13], part), 14)
    return {
        "latents": normal_values(part_keys[0], (LATENT, SAMPLES, D), 1.0, 6.0, ((0, 16),)),
        "context": normal_values(part_keys[1], (CTX, SAMPLES, D), 1.0, 6.0, ((0, 4),)),
        "condition": normal_values(part_keys[2], (SAMPLES, D), 1.0, 6.0, ((1, 4),), jnp.float32),
        "cond_context": normal_values(streams_of[3], (D,), 1.0, 6.0, ((0, 4),), jnp.float32),
        "w_shift": normal_values(streams_of[4], (D, D), D ** -0.5, 0.125, ((0, 4), (1, 4))),
        "w_scale": normal_values(streams_of[5], (D, D), D ** -0.5, 0.125, ((0, 4), (1, 4))),
        "w_gate": normal_values(streams_of[6], (D, D), (D // 8) ** -0.5, 0.375, ((0, 4), (1, 4))),
        "norm_gain": jnp.clip(1.0 + 0.18 * jax.random.normal(streams_of[7], (D,), jnp.float32), 0.1, 1.9),
        "w_query": normal_values(streams_of[8], (D, N_HEADS * HEAD_DIM), (D // 8) ** -0.5, 0.375, ((1, 4),)),
        "w_key": normal_values(streams_of[9], (D, N_KV * HEAD_DIM), D ** -0.5, 0.125, ((1, 4),)),
        "w_value": normal_values(streams_of[10], (D, N_KV * HEAD_DIM), (D // 4) ** -0.5, 0.25, ((1, 4),)),
        "sink_logit": draw_sink_logit(jax.random.fold_in(streams_of[13], 71), part),
        "w_out": normal_values(streams_of[12], (N_HEADS * HEAD_DIM, D), (N_HEADS * HEAD_DIM) ** -0.5, 0.1875, ((0, 4),)),
    }


EPS = 1e-06
THETA = 10000.0
BIG_NEG = -1e+30

def rotate_pairs(vectors, grid_row, grid_col, head_dim):
    quarter = head_dim // 4
    inverse = THETA ** (-jnp.arange(quarter, dtype=jnp.float32) / quarter)
    angles = jnp.concatenate([grid_row[:, None] * inverse, grid_col[:, None] * inverse], axis=-1)
    shape = (angles.shape[0],) + (1,) * (vectors.ndim - 2) + (head_dim // 2,)
    cosine = jnp.cos(angles).reshape(shape)
    sine = jnp.sin(angles).reshape(shape)
    first_half = vectors[..., :head_dim // 2]
    second_half = vectors[..., head_dim // 2:]
    return jnp.concatenate([first_half * cosine - second_half * sine, first_half * sine + second_half * cosine], axis=-1)

def modulate(tokens_in, gain, shift_rows, scale_rows):
    upcast = tokens_in.astype(jnp.float32)
    normed = upcast * lax.rsqrt(lax.optimization_barrier(jnp.mean(upcast * upcast, axis=-1, keepdims=True)) + EPS)
    return (normed * gain * (1.0 + scale_rows) + shift_rows).astype(jnp.bfloat16)

def reference(latents, context, condition, cond_context, w_shift, w_scale, w_gate, norm_gain, w_query, w_key, w_value, sink_logit, w_out):
    lifted = jax.nn.silu(jnp.concatenate([condition, cond_context[None, :]], axis=0)).astype(jnp.bfloat16)
    shift_all = jnp.dot(lifted, w_shift, preferred_element_type=jnp.float32)
    scale_all = jnp.dot(lifted, w_scale, preferred_element_type=jnp.float32)
    gate_all = jnp.dot(lifted, w_gate, preferred_element_type=jnp.float32)
    normed = modulate(latents, norm_gain, shift_all[:SAMPLES][None], scale_all[:SAMPLES][None])
    ctx_normed = modulate(context, norm_gain, shift_all[SAMPLES][None, None], scale_all[SAMPLES][None, None])
    flat_rows = normed.reshape(LATENT * SAMPLES, D)
    positions = jnp.arange(LATENT, dtype=jnp.int32)
    grid_row = (positions // GRID_W).astype(jnp.float32)
    grid_col = (positions % GRID_W).astype(jnp.float32)
    q_full = jnp.dot(flat_rows, w_query, preferred_element_type=jnp.float32).reshape(LATENT, SAMPLES, N_HEADS, HEAD_DIM)
    k_full = jnp.dot(flat_rows, w_key, preferred_element_type=jnp.float32).reshape(LATENT, SAMPLES, N_KV, HEAD_DIM)
    queries = rotate_pairs(q_full, grid_row, grid_col, HEAD_DIM).astype(jnp.bfloat16)
    lat_keys = rotate_pairs(k_full, grid_row, grid_col, HEAD_DIM).astype(jnp.bfloat16)
    lat_values = jnp.dot(flat_rows, w_value, preferred_element_type=jnp.float32).astype(jnp.bfloat16).reshape(LATENT, SAMPLES, N_KV, HEAD_DIM)
    ctx_flat = ctx_normed.reshape(CTX * SAMPLES, D)
    ctx_keys = jnp.dot(ctx_flat, w_key, preferred_element_type=jnp.float32).astype(jnp.bfloat16).reshape(CTX, SAMPLES, N_KV, HEAD_DIM)
    ctx_values = jnp.dot(ctx_flat, w_value, preferred_element_type=jnp.float32).astype(jnp.bfloat16).reshape(CTX, SAMPLES, N_KV, HEAD_DIM)
    per_group = N_HEADS // N_KV
    block_rows = min(TOK_DEV, 256)
    n_blocks = LATENT // block_rows
    padding = ((WINDOW, WINDOW), (0, 0), (0, 0), (0, 0))
    keys_padded = jnp.pad(lat_keys, padding)
    values_padded = jnp.pad(lat_values, padding)
    head_sinks = sink_logit.astype(jnp.float32).reshape(N_KV, per_group)
    score_scale = HEAD_DIM ** (-0.5)
    ctx_k32 = ctx_keys.astype(jnp.float32)
    ctx_v32 = ctx_values.astype(jnp.float32)

    def attend_block(block_index):
        first_row = block_index * block_rows
        q_blk = lax.dynamic_slice_in_dim(queries, first_row, block_rows, 0).reshape(block_rows, SAMPLES, N_KV, per_group, HEAD_DIM).astype(jnp.float32)
        k_blk = lax.dynamic_slice_in_dim(keys_padded, first_row, block_rows + 2 * WINDOW, 0).astype(jnp.float32)
        v_blk = lax.dynamic_slice_in_dim(values_padded, first_row, block_rows + 2 * WINDOW, 0).astype(jnp.float32)
        lat_scores = jnp.einsum('qsngd,ksnd->sngqk', q_blk, k_blk) * score_scale
        q_pos = first_row + jnp.arange(block_rows, dtype=jnp.int32)
        k_pos = first_row - WINDOW + jnp.arange(block_rows + 2 * WINDOW, dtype=jnp.int32)
        in_window = (jnp.abs(q_pos[:, None] - k_pos[None, :]) <= WINDOW) & (k_pos >= 0)[None, :] & (k_pos < LATENT)[None, :]
        lat_scores = jnp.where(in_window, lat_scores, BIG_NEG)
        ctx_scores = jnp.einsum('qsngd,ksnd->sngqk', q_blk, ctx_k32) * score_scale
        sink_col = jnp.broadcast_to(head_sinks[None, :, :, None, None], lat_scores.shape[:-1] + (1,))
        joined = jax.nn.softmax(jnp.concatenate([lat_scores, ctx_scores, sink_col], axis=-1), axis=-1)
        weights_low = joined.astype(jnp.bfloat16).astype(jnp.float32)
        lat_part = weights_low[..., :block_rows + 2 * WINDOW]
        ctx_part = weights_low[..., block_rows + 2 * WINDOW:block_rows + 2 * WINDOW + CTX]
        summed = jnp.einsum('sngqk,ksnd->qsngd', lat_part, v_blk) + jnp.einsum('sngqk,ksnd->qsngd', ctx_part, ctx_v32)
        return summed.astype(jnp.bfloat16).reshape(block_rows, SAMPLES, N_HEADS * HEAD_DIM)
    attended = lax.map(attend_block, jnp.arange(n_blocks)).reshape(LATENT * SAMPLES, N_HEADS * HEAD_DIM)
    group_cols = N_HEADS * HEAD_DIM // N_TP
    mixed = jnp.zeros((LATENT * SAMPLES, D), jnp.float32)
    for group_index in range(N_TP):
        lo_col = group_index * group_cols
        partial_term = jnp.dot(attended[:, lo_col:lo_col + group_cols], w_out[lo_col:lo_col + group_cols], preferred_element_type=jnp.float32)
        rounded = lax.optimization_barrier(partial_term.astype(jnp.bfloat16))
        mixed = mixed + rounded.astype(jnp.float32)
    mixed = mixed.reshape(LATENT, SAMPLES, D)
    refined = latents.astype(jnp.float32) + gate_all[:SAMPLES][None] * mixed
    return refined.astype(jnp.bfloat16)
```

```python
import functools

import jax
import jax.numpy as jnp
from jax import lax
from jax.experimental import pallas as pl
from jax.experimental.pallas import tpu as pltpu
from jax.sharding import PartitionSpec as P

HEAD_DIM = 64
WINDOW = 128
GRID_W = 64
LANES = 128
CORES = 2

EPS = 1e-06
THETA = 10000.0
BIG_NEG = -1e30


def peers(n_tp):
    return [(c, e) for c in range(n_tp // CORES) for e in range(CORES)]


def peer_perm(n_tp, c, e):
    chips = n_tp // CORES
    return [
        (i, ((i // CORES + c) % chips) * CORES + ((i % CORES) ^ e)) for i in range(n_tp)
    ]


def gather_tp(own, n_tp):
    blocks = {(0, 0): own}
    for c in range(1, n_tp // CORES):
        blocks[(c, 0)] = lax.ppermute(own, "tp", peer_perm(n_tp, c, 0))
    for c in range(n_tp // CORES):
        blocks[(c, 1)] = lax.ppermute(blocks[(c, 0)], "tp", peer_perm(n_tp, 0, 1))
    return [blocks[p] for p in peers(n_tp)]


def norm_rows(x, mult, add):
    up = x.astype(jnp.float32)
    r = lax.rsqrt(jnp.mean(up * up, axis=-1, keepdims=True) + EPS)
    return (up * r * mult + add).astype(jnp.bfloat16)


def ctx_kernel(x_ref, mult_ref, add_ref, wk_ref, wv_ref, out_ref):
    h = norm_rows(x_ref[0], mult_ref[...], add_ref[...])
    w = jnp.concatenate([wk_ref[...], wv_ref[...]], axis=1)
    out_ref[0] = jnp.dot(h, w, preferred_element_type=jnp.float32).astype(jnp.bfloat16)


def rotate(x, cos, sin, n_rot):
    lane = lax.broadcasted_iota(jnp.int32, x.shape, 1)
    half = HEAD_DIM // 2
    partner = jnp.where(
        lane % HEAD_DIM < half, pltpu.roll(x, LANES - half, 1), pltpu.roll(x, half, 1)
    )
    y = x * cos + partner * sin
    return y if n_rot >= LANES else jnp.where(lane < n_rot, y, x)


def proj_kernel(
    idx_ref, mult_ref, add_ref, cos_ref, sin_ref, wq_ref, wk_ref, wv_ref, *rest, n_src, scale
):
    xs = rest[:n_src]
    q_ref, kv_ref, buf, sems = rest[n_src:]
    copies = [pltpu.make_async_copy(xs[i], buf.at[i], sems.at[i]) for i in range(n_src)]
    for c in copies:
        c.start()
    samples, rows = buf.shape[1], buf.shape[2]
    q_cols = wq_ref.shape[1]
    rot_cols = q_cols + wk_ref.shape[1]
    w = jnp.concatenate([wq_ref[...], wk_ref[...], wv_ref[...]], axis=1)
    for i in range(n_src):
        copies[i].wait()
        h = jnp.concatenate(
            [norm_rows(buf[i, s], mult_ref[s : s + 1], add_ref[s : s + 1]) for s in range(samples)],
            axis=0,
        )
        y = jnp.dot(h, w, preferred_element_type=jnp.float32)
        at = pl.multiple_of(idx_ref[i] * rows, rows)
        cos = cos_ref[pl.ds(at, rows), :]
        sin = sin_ref[pl.ds(at, rows), :]
        for s in range(samples):
            for lo in range(0, w.shape[1], LANES):
                piece = y[s * rows : (s + 1) * rows, lo : lo + LANES]
                if lo < rot_cols:
                    piece = rotate(piece, cos, sin, rot_cols - lo)
                if lo < q_cols:
                    q_ref[s, pl.ds(at, rows), lo : lo + LANES] = (piece * scale).astype(
                        jnp.bfloat16
                    )
                else:
                    kv_ref[s, pl.ds(at, rows), lo - q_cols : lo - q_cols + LANES] = piece.astype(
                        jnp.bfloat16
                    )


def dot_t(a, b):
    return lax.dot_general(a, b, (((1,), (1,)), ((), ())), preferred_element_type=jnp.float32)


def attn_kernel(off_ref, sink_ref, q_ref, kv_ref, prev_ref, next_ref, *rest, n_ctx, seq, kv_cols):
    ctx = rest[:n_ctx]
    out_ref, ext = rest[n_ctx:]
    b = pl.program_id(0)
    block = q_ref.shape[1]
    tokens = kv_ref.shape[1]
    span = block + 2 * WINDOW

    @pl.when(b == 0)
    def _():
        ext[:WINDOW] = prev_ref[0]
        ext[WINDOW : WINDOW + tokens] = kv_ref[0]
        ext[WINDOW + tokens :] = next_ref[0]

    first = pl.multiple_of(b * block, block)
    r = lax.broadcasted_iota(jnp.int32, (block, span), 0)
    c = lax.broadcasted_iota(jnp.int32, (block, span), 1)
    pos = off_ref[0] + first - WINDOW + c
    ok = (c >= r) & (c <= r + 2 * WINDOW) & (pos >= 0) & (pos < seq)
    bias = jnp.where(ok, 0.0, BIG_NEG)
    local_kv = kv_cols // HEAD_DIM
    per_group = q_ref.shape[2] // kv_cols
    bias = jnp.concatenate([bias] * per_group, axis=0)
    kv_lat = ext[pl.ds(first, span), :]
    outs = []
    for n in range(local_kv):
        k_at = slice(n * HEAD_DIM, (n + 1) * HEAD_DIM)
        v_at = slice(kv_cols + n * HEAD_DIM, kv_cols + (n + 1) * HEAD_DIM)
        heads = [n * per_group + g for g in range(per_group)]
        q = jnp.concatenate(
            [q_ref[0, :, h * HEAD_DIM : (h + 1) * HEAD_DIM] for h in heads], axis=0
        )
        sink = jnp.concatenate(
            [jnp.full((block, 1), sink_ref[h], jnp.float32) for h in heads], axis=0
        )
        parts = [dot_t(q, kv_lat[:, k_at]) + bias]
        parts += [dot_t(q, t[0, :, k_at]) for t in ctx]
        vals = [kv_lat[:, v_at]] + [t[0, :, v_at] for t in ctx]
        top = sink
        for p in parts:
            top = jnp.maximum(top, jnp.max(p, axis=-1, keepdims=True))
        acc = jnp.zeros((block * per_group, 2 * HEAD_DIM), jnp.float32)
        for p, v in zip(parts, vals):
            e = jnp.exp(p - top).astype(jnp.bfloat16)
            va = jnp.concatenate([v, jnp.ones_like(v)], axis=1)
            acc = acc + jnp.dot(e, va, preferred_element_type=jnp.float32)
        den = acc[:, HEAD_DIM:] + jnp.exp(sink - top)
        o = (acc[:, :HEAD_DIM] / den).astype(jnp.bfloat16)
        outs += [o[g * block : (g + 1) * block] for g in range(per_group)]
    out_ref[...] = jnp.concatenate(outs, axis=1)


def out_kernel(*refs, n_src, samples):
    a = refs[: n_src * samples]
    w = refs[n_src * samples : n_src * (samples + 1)]
    gate_ref, lat_ref, out_ref = refs[n_src * (samples + 1) :]
    rows = lat_ref.shape[1]
    acc = None
    for k in range(n_src):
        lhs = jnp.concatenate([a[s * n_src + k][...] for s in range(samples)], axis=0)
        part = jnp.dot(lhs, w[k][...], preferred_element_type=jnp.float32)
        acc = part if acc is None else acc + part
    for s in range(samples):
        res = lat_ref[s].astype(jnp.float32) + gate_ref[s : s + 1] * acc[s * rows : (s + 1) * rows]
        out_ref[s] = res.astype(jnp.bfloat16)


def full(shape):
    zeros = (0,) * len(shape)
    return pl.BlockSpec(shape, lambda *_: zeros)


def on_device(
    latents,
    context,
    condition,
    cond_context,
    w_shift,
    w_scale,
    w_gate,
    norm_gain,
    w_query,
    w_key,
    w_value,
    sink_logit,
    w_out,
):
    rows, samples, width = latents.shape
    n_tp = lax.axis_size("tp")
    n_sp = lax.axis_size("sp")
    tokens = rows * n_tp
    q_cols = w_query.shape[1]
    kv_cols = w_key.shape[1]
    tp_i = lax.axis_index("tp")
    sp_i = lax.axis_index("sp")
    chips = n_tp // CORES
    order = peers(n_tp)

    lat_t = jnp.swapaxes(latents, 0, 1)
    lat_blocks = gather_tp(lat_t, n_tp)

    lifted = jax.nn.silu(jnp.concatenate([condition, cond_context[None, :]], axis=0)).astype(
        jnp.bfloat16
    )
    partial = jnp.stack(
        [jnp.dot(lifted, w, preferred_element_type=jnp.float32) for w in (w_shift, w_scale, w_gate)]
    )
    mods = lax.all_gather(partial, ("sp", "tp"), axis=0)
    mods = mods.reshape((n_sp, n_tp) + partial.shape).sum(axis=0)
    mods = jnp.moveaxis(mods, 0, 2).reshape(3, samples + 1, width)
    add_all = mods[0]
    mult_all = norm_gain[None] * (1.0 + mods[1])
    gate = mods[2, :samples]

    ctx_t = jnp.swapaxes(context, 0, 1)
    ctx_rows = context.shape[0]
    ctx_kv = pl.pallas_call(
        ctx_kernel,
        grid=(samples,),
        in_specs=[
            pl.BlockSpec((1, ctx_rows, width), lambda s: (s, 0, 0)),
            full((1, width)),
            full((1, width)),
            full(w_key.shape),
            full(w_value.shape),
        ],
        out_specs=pl.BlockSpec((1, ctx_rows, 2 * kv_cols), lambda s: (s, 0, 0)),
        out_shape=jax.ShapeDtypeStruct((samples, ctx_rows, 2 * kv_cols), jnp.bfloat16),
        name="ctx_proj",
    )(ctx_t, mult_all[samples:], add_all[samples:], w_key, w_value)
    ctx_blocks = [ctx_kv] + [
        lax.ppermute(ctx_kv, "sp", [(i, (i + k) % n_sp) for i in range(n_sp)])
        for k in range(1, n_sp)
    ]

    offset = sp_i * tokens
    positions = offset + jnp.arange(tokens, dtype=jnp.int32)
    quarter = HEAD_DIM // 4
    lane = jnp.arange(LANES, dtype=jnp.int32)
    inverse = THETA ** (-(lane % quarter).astype(jnp.float32) / quarter)
    is_row = (lane % (2 * quarter) < quarter)[None]
    grid_row = (positions // GRID_W).astype(jnp.float32)[:, None]
    grid_col = (positions % GRID_W).astype(jnp.float32)[:, None]
    angles = jnp.where(is_row, grid_row, grid_col) * inverse[None]
    cosine = jnp.cos(angles)
    sine = jnp.sin(angles) * jnp.where(lane % HEAD_DIM < HEAD_DIM // 2, -1.0, 1.0)[None]

    src = jnp.stack(
        [((tp_i // CORES - c) % chips) * CORES + ((tp_i % CORES) ^ e) for c, e in order]
    ).astype(jnp.int32)
    smem = pl.BlockSpec(memory_space=pltpu.SMEM)
    vmem = pl.BlockSpec(memory_space=pltpu.VMEM)
    queries, lat_kv = pl.pallas_call(
        functools.partial(proj_kernel, n_src=n_tp, scale=HEAD_DIM**-0.5),
        in_specs=[smem] + [vmem] * 7 + [pl.BlockSpec(memory_space=pl.ANY)] * n_tp,
        out_specs=[vmem, vmem],
        out_shape=[
            jax.ShapeDtypeStruct((samples, tokens, q_cols), jnp.bfloat16),
            jax.ShapeDtypeStruct((samples, tokens, 2 * kv_cols), jnp.bfloat16),
        ],
        scratch_shapes=[
            pltpu.VMEM((n_tp, samples, rows, width), jnp.bfloat16),
            pltpu.SemaphoreType.DMA((n_tp,)),
        ],
        name="lat_proj",
    )(
        src,
        mult_all[:samples],
        add_all[:samples],
        cosine,
        sine,
        w_query,
        w_key,
        w_value,
        *lat_blocks,
    )

    ends = n_sp - 1
    before = lax.ppermute(lat_kv[:, tokens - WINDOW :], "sp", [(i, i + 1) for i in range(ends)])
    after = lax.ppermute(lat_kv[:, :WINDOW], "sp", [(i + 1, i) for i in range(ends)])

    w_blocks = gather_tp(w_out, n_tp)

    block = min(tokens, 256)
    received = []
    for s in range(samples):
        part = functools.partial(lambda s, *_: (s, 0, 0), s)
        attended = pl.pallas_call(
            functools.partial(attn_kernel, n_ctx=n_sp, seq=tokens * n_sp, kv_cols=kv_cols),
            grid=(tokens // block,),
            in_specs=[
                smem,
                smem,
                pl.BlockSpec((1, block, q_cols), functools.partial(lambda s, b: (s, b, 0), s)),
                pl.BlockSpec((1, tokens, 2 * kv_cols), part),
                pl.BlockSpec((1, WINDOW, 2 * kv_cols), part),
                pl.BlockSpec((1, WINDOW, 2 * kv_cols), part),
            ]
            + [pl.BlockSpec((1, ctx_rows, 2 * kv_cols), part)] * n_sp,
            out_specs=pl.BlockSpec((block, q_cols), lambda b: (b, 0)),
            out_shape=jax.ShapeDtypeStruct((tokens, q_cols), jnp.bfloat16),
            scratch_shapes=[pltpu.VMEM((tokens + 2 * WINDOW, 2 * kv_cols), jnp.bfloat16)],
            name="attend",
        )(offset.reshape(1), sink_logit, queries, lat_kv, before, after, *ctx_blocks)
        for c, e in order:
            to = ((tp_i // CORES + c) % chips) * CORES + ((tp_i % CORES) ^ e)
            chunk = lax.dynamic_slice_in_dim(attended, to * rows, rows, axis=0)
            if (c, e) != (0, 0):
                chunk = lax.ppermute(chunk, "tp", peer_perm(n_tp, c, e))
            received.append(chunk)

    cols = min(width, 512)
    refined = pl.pallas_call(
        functools.partial(out_kernel, n_src=n_tp, samples=samples),
        grid=(width // cols,),
        in_specs=[full((rows, q_cols))] * (n_tp * samples)
        + [pl.BlockSpec((q_cols, cols), lambda j: (0, j))] * n_tp
        + [
            pl.BlockSpec((samples, cols), lambda j: (0, j)),
            pl.BlockSpec((samples, rows, cols), lambda j: (0, 0, j)),
        ],
        out_specs=pl.BlockSpec((samples, rows, cols), lambda j: (0, 0, j)),
        out_shape=jax.ShapeDtypeStruct((samples, rows, width), jnp.bfloat16),
        name="out_proj",
    )(*received, *w_blocks, gate, lat_t)
    return jnp.swapaxes(refined, 0, 1)


def solution(mesh):
    return jax.shard_map(
        on_device,
        mesh=mesh,
        in_specs=(
            P(("sp", "tp"), "grp", None),
            P("sp", "grp", None),
            P("grp", "sp"),
            P("sp"),
            P("sp", "tp"),
            P("sp", "tp"),
            P("sp", "tp"),
            P(),
            P(None, "tp"),
            P(None, "tp"),
            P(None, "tp"),
            P("tp"),
            P("tp", None),
        ),
        out_specs=P(("sp", "tp"), "grp", None),
        check_vma=False,
    )
```

```python
import functools

import jax
import jax.numpy as jnp
from jax import lax
from jax.experimental import pallas as pl
from jax.experimental.pallas import tpu as pltpu
from jax.sharding import PartitionSpec as P

HEAD_DIM = 64
WINDOW = 128
GRID_W = 64
LANES = 128
CORES = 2

EPS = 1e-06
THETA = 10000.0
BIG_NEG = -1e30


def peers(n_tp):
    return [(c, e) for c in range(n_tp // CORES) for e in range(CORES)]


def peer_perm(n_tp, c, e):
    chips = n_tp // CORES
    return [
        (i, ((i // CORES + c) % chips) * CORES + ((i % CORES) ^ e)) for i in range(n_tp)
    ]


def across_chips(own, n_tp):
    return [own] + [
        lax.ppermute(own, "tp", peer_perm(n_tp, c, 0)) for c in range(1, n_tp // CORES)
    ]


def across_cores(blocks, n_tp):
    out = []
    for block in blocks:
        out += [block, lax.ppermute(block, "tp", peer_perm(n_tp, 0, 1))]
    return out


def norm_rows(x, mult, add):
    up = x.astype(jnp.float32)
    r = lax.rsqrt(jnp.mean(up * up, axis=-1, keepdims=True) + EPS)
    return (up * r * mult + add).astype(jnp.bfloat16)


def mod_kernel(cond_ref, ctx_ref, shift_ref, scale_ref, gate_ref, out_ref):
    lift = jnp.concatenate([cond_ref[...], ctx_ref[...]], axis=0)
    lift = (lift / (1.0 + jnp.exp(-lift))).astype(jnp.bfloat16)
    n = lift.shape[0]
    out_ref[0:n] = jnp.dot(lift, shift_ref[...], preferred_element_type=jnp.float32)
    out_ref[n : 2 * n] = jnp.dot(lift, scale_ref[...], preferred_element_type=jnp.float32)
    gate = jnp.dot(lift, gate_ref[...], preferred_element_type=jnp.float32)
    out_ref[2 * n : 3 * n - 1] = gate[: n - 1]


def mod_rows(at_ref, refs):
    parts = []
    for j in range(refs[0].shape[0]):
        k = at_ref[j]
        total = refs[0][k]
        for ref in refs[1:]:
            total = total + ref[k]
        parts.append(total)
    return jnp.concatenate(parts, axis=1)


def ctx_kernel(at_ref, x_ref, gain_ref, wk_ref, wv_ref, *rest):
    out_ref = rest[-1]
    rows = mod_rows(at_ref, rest[:-1])
    n = (rows.shape[0] + 1) // 3
    add = rows[n - 1 : n]
    mult = gain_ref[...] * (1.0 + rows[2 * n - 1 : 2 * n])
    h = norm_rows(x_ref[0], mult, add)
    w = jnp.concatenate([wk_ref[...], wv_ref[...]], axis=1)
    out_ref[0] = jnp.dot(h, w, preferred_element_type=jnp.float32).astype(jnp.bfloat16)


def rotate(x, cos, sin, n_rot):
    lane = lax.broadcasted_iota(jnp.int32, x.shape, 1)
    half = HEAD_DIM // 2
    partner = jnp.where(
        lane % HEAD_DIM < half, pltpu.roll(x, LANES - half, 1), pltpu.roll(x, half, 1)
    )
    y = x * cos + partner * sin
    return y if n_rot >= LANES else jnp.where(lane < n_rot, y, x)


def proj_kernel(
    idx_ref, at_ref, gain_ref, cos_ref, sin_ref, wq_ref, wk_ref, wv_ref, *rest, n_src, n_mod, scale
):
    xs = rest[:n_src]
    mods = rest[n_src : n_src + n_mod]
    q_ref, kv_ref, buf, sems = rest[n_src + n_mod :]
    copies = [pltpu.make_async_copy(xs[i], buf.at[i], sems.at[i]) for i in range(n_src)]
    for c in copies:
        c.start()
    samples, rows = buf.shape[1], buf.shape[2]
    q_cols = wq_ref.shape[1]
    rot_cols = q_cols + wk_ref.shape[1]
    w = jnp.concatenate([wq_ref[...], wk_ref[...], wv_ref[...]], axis=1)
    mod = mod_rows(at_ref, mods)
    n = samples + 1
    add = mod[:samples]
    mult = gain_ref[...] * (1.0 + mod[n : n + samples])
    for i in range(n_src):
        copies[i].wait()
        h = jnp.concatenate(
            [norm_rows(buf[i, s], mult[s : s + 1], add[s : s + 1]) for s in range(samples)],
            axis=0,
        )
        y = jnp.dot(h, w, preferred_element_type=jnp.float32)
        at = pl.multiple_of(idx_ref[i] * rows, rows)
        cos = cos_ref[pl.ds(at, rows), :]
        sin = sin_ref[pl.ds(at, rows), :]
        for s in range(samples):
            for lo in range(0, w.shape[1], LANES):
                piece = y[s * rows : (s + 1) * rows, lo : lo + LANES]
                if lo < rot_cols:
                    piece = rotate(piece, cos, sin, rot_cols - lo)
                if lo < q_cols:
                    q_ref[s, pl.ds(at, rows), lo : lo + LANES] = (piece * scale).astype(
                        jnp.bfloat16
                    )
                else:
                    kv_ref[s, pl.ds(at, rows), lo - q_cols : lo - q_cols + LANES] = piece.astype(
                        jnp.bfloat16
                    )


def dot_t(a, b):
    return lax.dot_general(a, b, (((1,), (1,)), ((), ())), preferred_element_type=jnp.float32)


def interior_kernel(sink_ref, q_ref, kv_ref, *rest, kv_cols):
    ctx, out_ref = rest[:-1], rest[-1]
    block = q_ref.shape[1] - 2 * WINDOW
    q = q_ref[0, WINDOW : WINDOW + block]
    out_ref[...] = attend(sink_ref, q, kv_ref[0], ctx, None, kv_cols)


def edge_kernel(sp_ref, sink_ref, q_ref, kv_ref, prev_ref, next_ref, *rest, kv_cols, n_sp):
    ctx, out_ref = rest[:-1], rest[-1]
    tokens = q_ref.shape[1]
    pos = lax.broadcasted_iota(jnp.int32, (WINDOW, 3 * WINDOW), 1)
    kv = jnp.concatenate([prev_ref[0], kv_ref[0, : 2 * WINDOW]], axis=0)
    ok = (pos >= WINDOW) | (sp_ref[0] > 0)
    out_ref[:WINDOW] = attend(sink_ref, q_ref[0, :WINDOW], kv, ctx, ok, kv_cols)
    kv = jnp.concatenate([kv_ref[0, tokens - 2 * WINDOW :], next_ref[0]], axis=0)
    ok = (pos < 2 * WINDOW) | (sp_ref[0] < n_sp - 1)
    out_ref[WINDOW:] = attend(sink_ref, q_ref[0, tokens - WINDOW :], kv, ctx, ok, kv_cols)


def attend(sink_ref, queries, kv_lat, ctx, inside, kv_cols):
    block = queries.shape[0]
    span = kv_lat.shape[0]
    r = lax.broadcasted_iota(jnp.int32, (block, span), 0)
    c = lax.broadcasted_iota(jnp.int32, (block, span), 1)
    ok = (c >= r) & (c <= r + 2 * WINDOW)
    if inside is not None:
        ok = ok & inside
    bias = jnp.where(ok, 0.0, BIG_NEG)
    local_kv = kv_cols // HEAD_DIM
    per_group = queries.shape[1] // kv_cols
    bias = jnp.concatenate([bias] * per_group, axis=0)
    outs = []
    for n in range(local_kv):
        k_at = slice(n * HEAD_DIM, (n + 1) * HEAD_DIM)
        v_at = slice(kv_cols + n * HEAD_DIM, kv_cols + (n + 1) * HEAD_DIM)
        heads = [n * per_group + g for g in range(per_group)]
        q = jnp.concatenate(
            [queries[:, h * HEAD_DIM : (h + 1) * HEAD_DIM] for h in heads], axis=0
        )
        sink = jnp.concatenate(
            [jnp.full((block, 1), sink_ref[h], jnp.float32) for h in heads], axis=0
        )
        parts = [dot_t(q, kv_lat[:, k_at]) + bias]
        parts += [dot_t(q, t[0, :, k_at]) for t in ctx]
        vals = [kv_lat[:, v_at]] + [t[0, :, v_at] for t in ctx]
        top = sink
        for p in parts:
            top = jnp.maximum(top, jnp.max(p, axis=-1, keepdims=True))
        acc = jnp.zeros((block * per_group, 2 * HEAD_DIM), jnp.float32)
        for p, v in zip(parts, vals):
            e = jnp.exp(p - top).astype(jnp.bfloat16)
            va = jnp.concatenate([v, jnp.ones_like(v)], axis=1)
            acc = acc + jnp.dot(e, va, preferred_element_type=jnp.float32)
        den = acc[:, HEAD_DIM:] + jnp.exp(sink - top)
        o = (acc[:, :HEAD_DIM] / den).astype(jnp.bfloat16)
        outs += [o[g * block : (g + 1) * block] for g in range(per_group)]
    return jnp.concatenate(outs, axis=1)


def out_kernel(*refs, n_src, samples):
    a = refs[: n_src * samples]
    w = refs[n_src * samples : n_src * (samples + 1)]
    at_ref, lat_ref, *mods, out_ref = refs[n_src * (samples + 1) :]
    total = mods[0][at_ref[pl.program_id(0)]]
    for ref in mods[1:]:
        total = total + ref[at_ref[pl.program_id(0)]]
    gate = total[2 * (samples + 1) :]
    rows = lat_ref.shape[1]
    acc = None
    for k in range(n_src):
        lhs = jnp.concatenate([a[s * n_src + k][...] for s in range(samples)], axis=0)
        part = jnp.dot(lhs, w[k][...], preferred_element_type=jnp.float32)
        acc = part if acc is None else acc + part
    for s in range(samples):
        res = lat_ref[s].astype(jnp.float32) + gate[s : s + 1] * acc[s * rows : (s + 1) * rows]
        out_ref[s] = res.astype(jnp.bfloat16)


def full(shape):
    zeros = (0,) * len(shape)
    return pl.BlockSpec(shape, lambda *_: zeros)


def on_device(
    latents,
    context,
    condition,
    cond_context,
    w_shift,
    w_scale,
    w_gate,
    norm_gain,
    w_query,
    w_key,
    w_value,
    sink_logit,
    w_out,
):
    rows, samples, width = latents.shape
    n_tp = lax.axis_size("tp")
    n_sp = lax.axis_size("sp")
    tokens = rows * n_tp
    q_cols = w_query.shape[1]
    kv_cols = w_key.shape[1]
    tp_i = lax.axis_index("tp")
    sp_i = lax.axis_index("sp")
    chips = n_tp // CORES
    order = peers(n_tp)

    smem = pl.BlockSpec(memory_space=pltpu.SMEM)
    vmem = pl.BlockSpec(memory_space=pltpu.VMEM)
    features = w_shift.shape[1]
    n_rows = 3 * samples + 2
    part = pl.pallas_call(
        mod_kernel,
        in_specs=[vmem] * 5,
        out_specs=vmem,
        out_shape=jax.ShapeDtypeStruct((n_rows, features), jnp.float32),
        name="mod_dots",
    )(condition, cond_context[None, :], w_shift, w_scale, w_gate)
    pieces = [
        part if p == (0, 0) else lax.ppermute(part, "tp", peer_perm(n_tp, *p)) for p in order
    ]
    lat_t = jnp.swapaxes(latents, 0, 1)
    lat_own, pieces = lax.optimization_barrier((lat_t, pieces))
    lat_far = across_chips(lat_own, n_tp)
    own_mods = jnp.stack(pieces)
    mods = [own_mods] + [
        lax.ppermute(own_mods, "sp", [(i, (i + k) % n_sp) for i in range(n_sp)])
        for k in range(1, n_sp)
    ]
    at = jnp.stack(
        [
            ((tp_i // CORES - j // CORES) % chips) * CORES + ((tp_i % CORES) ^ (j % CORES))
            for j in range(n_tp)
        ]
    ).astype(jnp.int32)
    gain = norm_gain[None]

    ctx_t = jnp.swapaxes(context, 0, 1)
    ctx_rows = context.shape[0]
    ctx_kv = pl.pallas_call(
        ctx_kernel,
        grid=(samples,),
        in_specs=[
            smem,
            pl.BlockSpec((1, ctx_rows, width), lambda s: (s, 0, 0)),
            full((1, width)),
            full(w_key.shape),
            full(w_value.shape),
        ]
        + [full(own_mods.shape)] * n_sp,
        out_specs=pl.BlockSpec((1, ctx_rows, 2 * kv_cols), lambda s: (s, 0, 0)),
        out_shape=jax.ShapeDtypeStruct((samples, ctx_rows, 2 * kv_cols), jnp.bfloat16),
        name="ctx_proj",
    )(at, ctx_t, gain, w_key, w_value, *mods)
    ctx_blocks = [ctx_kv] + [
        lax.ppermute(ctx_kv, "sp", [(i, (i + k) % n_sp) for i in range(n_sp)])
        for k in range(1, n_sp)
    ]

    offset = sp_i * tokens
    positions = offset + jnp.arange(tokens, dtype=jnp.int32)
    quarter = HEAD_DIM // 4
    lane = jnp.arange(LANES, dtype=jnp.int32)
    inverse = THETA ** (-(lane % quarter).astype(jnp.float32) / quarter)
    is_row = (lane % (2 * quarter) < quarter)[None]
    grid_row = (positions // GRID_W).astype(jnp.float32)[:, None]
    grid_col = (positions % GRID_W).astype(jnp.float32)[:, None]
    angles = jnp.where(is_row, grid_row, grid_col) * inverse[None]
    cosine = jnp.cos(angles)
    sine = jnp.sin(angles) * jnp.where(lane % HEAD_DIM < HEAD_DIM // 2, -1.0, 1.0)[None]

    lat_far, ctx_blocks, cosine, sine = lax.optimization_barrier(
        (lat_far, ctx_blocks, cosine, sine)
    )
    lat_blocks = across_cores(lat_far, n_tp)

    src = jnp.stack(
        [((tp_i // CORES - c) % chips) * CORES + ((tp_i % CORES) ^ e) for c, e in order]
    ).astype(jnp.int32)
    queries, lat_kv = pl.pallas_call(
        functools.partial(proj_kernel, n_src=n_tp, n_mod=n_sp, scale=HEAD_DIM**-0.5),
        in_specs=[smem, smem]
        + [vmem] * 6
        + [pl.BlockSpec(memory_space=pl.ANY)] * n_tp
        + [vmem] * n_sp,
        out_specs=[vmem, vmem],
        out_shape=[
            jax.ShapeDtypeStruct((samples, tokens, q_cols), jnp.bfloat16),
            jax.ShapeDtypeStruct((samples, tokens, 2 * kv_cols), jnp.bfloat16),
        ],
        scratch_shapes=[
            pltpu.VMEM((n_tp, samples, rows, width), jnp.bfloat16),
            pltpu.SemaphoreType.DMA((n_tp,)),
        ],
        name="lat_proj",
    )(
        src,
        at,
        gain,
        cosine,
        sine,
        w_query,
        w_key,
        w_value,
        *lat_blocks,
        *mods,
    )

    ends = n_sp - 1
    before = lax.ppermute(lat_kv[:, tokens - WINDOW :], "sp", [(i, i + 1) for i in range(ends)])
    after = lax.ppermute(lat_kv[:, :WINDOW], "sp", [(i + 1, i) for i in range(ends)])

    w_own, _ = lax.optimization_barrier((w_out, lat_far))
    w_far = across_chips(w_own, n_tp)

    inner = []
    for s in range(samples):
        part_at = functools.partial(lambda s, *_: (s, 0, 0), s)
        own_specs = [
            pl.BlockSpec((1, tokens, q_cols), part_at),
            pl.BlockSpec((1, tokens, 2 * kv_cols), part_at),
        ]
        ctx_specs = [pl.BlockSpec((1, ctx_rows, 2 * kv_cols), part_at)] * n_sp
        inner.append(
            pl.pallas_call(
                functools.partial(interior_kernel, kv_cols=kv_cols),
                grid=(1,),
                in_specs=[smem] + own_specs + ctx_specs,
                out_specs=full((tokens - 2 * WINDOW, q_cols)),
                out_shape=jax.ShapeDtypeStruct((tokens - 2 * WINDOW, q_cols), jnp.bfloat16),
                name="attend_inner",
            )(sink_logit, queries, lat_kv, *ctx_blocks)
        )
    before, after, inner, w_far = lax.optimization_barrier((before, after, inner, w_far))
    w_blocks = across_cores(w_far, n_tp)
    received = []
    for s in range(samples):
        part_at = functools.partial(lambda s, *_: (s, 0, 0), s)
        own_specs = [
            pl.BlockSpec((1, tokens, q_cols), part_at),
            pl.BlockSpec((1, tokens, 2 * kv_cols), part_at),
        ]
        ctx_specs = [pl.BlockSpec((1, ctx_rows, 2 * kv_cols), part_at)] * n_sp
        edges = pl.pallas_call(
            functools.partial(edge_kernel, kv_cols=kv_cols, n_sp=n_sp),
            grid=(1,),
            in_specs=[smem, smem]
            + own_specs
            + [pl.BlockSpec((1, WINDOW, 2 * kv_cols), part_at)] * 2
            + ctx_specs,
            out_specs=full((2 * WINDOW, q_cols)),
            out_shape=jax.ShapeDtypeStruct((2 * WINDOW, q_cols), jnp.bfloat16),
            name="attend_edges",
        )(sp_i.reshape(1), sink_logit, queries, lat_kv, before, after, *ctx_blocks)
        attended = jnp.concatenate([edges[:WINDOW], inner[s], edges[WINDOW:]], axis=0)
        for c, e in order:
            to = ((tp_i // CORES + c) % chips) * CORES + ((tp_i % CORES) ^ e)
            chunk = lax.dynamic_slice_in_dim(attended, to * rows, rows, axis=0)
            if (c, e) != (0, 0):
                chunk = lax.ppermute(chunk, "tp", peer_perm(n_tp, c, e))
            received.append(chunk)

    cols = features
    refined = pl.pallas_call(
        functools.partial(out_kernel, n_src=n_tp, samples=samples),
        grid=(width // cols,),
        in_specs=[full((rows, q_cols))] * (n_tp * samples)
        + [pl.BlockSpec((q_cols, cols), lambda j: (0, j))] * n_tp
        + [
            smem,
            pl.BlockSpec((samples, rows, cols), lambda j: (0, 0, j)),
        ]
        + [full(own_mods.shape)] * n_sp,
        out_specs=pl.BlockSpec((samples, rows, cols), lambda j: (0, 0, j)),
        out_shape=jax.ShapeDtypeStruct((samples, rows, width), jnp.bfloat16),
        name="out_proj",
    )(*received, *w_blocks, at, lat_t, *mods)
    return jnp.swapaxes(refined, 0, 1)


def solution(mesh):
    return jax.shard_map(
        on_device,
        mesh=mesh,
        in_specs=(
            P(("sp", "tp"), "grp", None),
            P("sp", "grp", None),
            P("grp", "sp"),
            P("sp"),
            P("sp", "tp"),
            P("sp", "tp"),
            P("sp", "tp"),
            P(),
            P(None, "tp"),
            P(None, "tp"),
            P(None, "tp"),
            P("tp"),
            P("tp", None),
        ),
        out_specs=P(("sp", "tp"), "grp", None),
        check_vma=False,
    )
```

```python
import functools

import jax
import jax.numpy as jnp
from jax import lax
from jax.experimental import pallas as pl
from jax.experimental.pallas import tpu as pltpu
from jax.sharding import PartitionSpec as P

HEAD_DIM = 64
WINDOW = 128
GRID_W = 64
LANES = 128
CORES = 2

EPS = 1e-06
THETA = 10000.0
BIG_NEG = -1e30


def peers(n_tp):
    return [(c, e) for c in range(n_tp // CORES) for e in range(CORES)]


def peer_perm(n_tp, c, e):
    chips = n_tp // CORES
    return [
        (i, ((i // CORES + c) % chips) * CORES + ((i % CORES) ^ e)) for i in range(n_tp)
    ]


def across_chips(own, n_tp):
    return [own] + [
        lax.ppermute(own, "tp", peer_perm(n_tp, c, 0)) for c in range(1, n_tp // CORES)
    ]


def across_cores(blocks, n_tp):
    out = []
    for block in blocks:
        out += [block, lax.ppermute(block, "tp", peer_perm(n_tp, 0, 1))]
    return out


def norm_rows(x, mult, add):
    up = x.astype(jnp.float32)
    r = lax.rsqrt(jnp.mean(up * up, axis=-1, keepdims=True) + EPS)
    return (up * r * mult + add).astype(jnp.bfloat16)


def mod_kernel(cond_ref, ctx_ref, shift_ref, scale_ref, gate_ref, out_ref):
    lift = jnp.concatenate([cond_ref[...], ctx_ref[...]], axis=0)
    lift = (lift / (1.0 + jnp.exp(-lift))).astype(jnp.bfloat16)
    n = lift.shape[0]
    out_ref[0:n] = jnp.dot(lift, shift_ref[...], preferred_element_type=jnp.float32)
    out_ref[n : 2 * n] = jnp.dot(lift, scale_ref[...], preferred_element_type=jnp.float32)
    gate = jnp.dot(lift, gate_ref[...], preferred_element_type=jnp.float32)
    out_ref[2 * n : 3 * n - 1] = gate[: n - 1]


def mod_rows(at_ref, refs):
    parts = []
    for j in range(refs[0].shape[0]):
        k = at_ref[j]
        total = refs[0][k]
        for ref in refs[1:]:
            total = total + ref[k]
        parts.append(total)
    return jnp.concatenate(parts, axis=1)


def ctx_kernel(at_ref, x_ref, gain_ref, wk_ref, wv_ref, *rest):
    out_ref = rest[-1]
    rows = mod_rows(at_ref, rest[:-1])
    n = (rows.shape[0] + 1) // 3
    add = rows[n - 1 : n]
    mult = gain_ref[...] * (1.0 + rows[2 * n - 1 : 2 * n])
    h = norm_rows(x_ref[0], mult, add)
    w = jnp.concatenate([wk_ref[...], wv_ref[...]], axis=1)
    out_ref[0] = jnp.dot(h, w, preferred_element_type=jnp.float32).astype(jnp.bfloat16)


def rotate(x, cos, sin, n_rot):
    lane = lax.broadcasted_iota(jnp.int32, x.shape, 1)
    half = HEAD_DIM // 2
    partner = jnp.where(
        lane % HEAD_DIM < half, pltpu.roll(x, LANES - half, 1), pltpu.roll(x, half, 1)
    )
    y = x * cos + partner * sin
    return y if n_rot >= LANES else jnp.where(lane < n_rot, y, x)


def proj_kernel(
    idx_ref, at_ref, gain_ref, cos_ref, sin_ref, wq_ref, wk_ref, wv_ref, *rest, n_src, n_mod, scale
):
    xs = rest[:n_src]
    mods = rest[n_src : n_src + n_mod]
    q_ref, kv_ref, buf, sems = rest[n_src + n_mod :]
    copies = [pltpu.make_async_copy(xs[i], buf.at[i], sems.at[i]) for i in range(n_src)]
    for c in copies:
        c.start()
    samples, rows = buf.shape[1], buf.shape[2]
    q_cols = wq_ref.shape[1]
    rot_cols = q_cols + wk_ref.shape[1]
    w = jnp.concatenate([wq_ref[...], wk_ref[...], wv_ref[...]], axis=1)
    mod = mod_rows(at_ref, mods)
    n = samples + 1
    add = mod[:samples]
    mult = gain_ref[...] * (1.0 + mod[n : n + samples])
    for i in range(n_src):
        copies[i].wait()
        h = jnp.concatenate(
            [norm_rows(buf[i, s], mult[s : s + 1], add[s : s + 1]) for s in range(samples)],
            axis=0,
        )
        y = jnp.dot(h, w, preferred_element_type=jnp.float32)
        at = pl.multiple_of(idx_ref[i] * rows, rows)
        cos = cos_ref[pl.ds(at, rows), :]
        sin = sin_ref[pl.ds(at, rows), :]
        for s in range(samples):
            for lo in range(0, w.shape[1], LANES):
                piece = y[s * rows : (s + 1) * rows, lo : lo + LANES]
                if lo < rot_cols:
                    piece = rotate(piece, cos, sin, rot_cols - lo)
                if lo < q_cols:
                    q_ref[s, pl.ds(at, rows), lo : lo + LANES] = (piece * scale).astype(
                        jnp.bfloat16
                    )
                else:
                    kv_ref[s, pl.ds(at, rows), lo - q_cols : lo - q_cols + LANES] = piece.astype(
                        jnp.bfloat16
                    )


def dot_t(a, b):
    return lax.dot_general(a, b, (((1,), (1,)), ((), ())), preferred_element_type=jnp.float32)


def interior_kernel(sink_ref, q_ref, kv_ref, *rest, kv_cols):
    ctx, out_ref = rest[:-1], rest[-1]
    block = q_ref.shape[1] - 2 * WINDOW
    q = q_ref[0, WINDOW : WINDOW + block]
    out_ref[...] = attend(sink_ref, q, kv_ref[0], ctx, None, kv_cols)


def edge_kernel(sp_ref, sink_ref, q_ref, kv_ref, prev_ref, next_ref, *rest, kv_cols, n_sp):
    ctx, out_ref = rest[:-1], rest[-1]
    tokens = q_ref.shape[1]
    pos = lax.broadcasted_iota(jnp.int32, (WINDOW, 3 * WINDOW), 1)
    kv = jnp.concatenate([prev_ref[0], kv_ref[0, : 2 * WINDOW]], axis=0)
    ok = (pos >= WINDOW) | (sp_ref[0] > 0)
    out_ref[:WINDOW] = attend(sink_ref, q_ref[0, :WINDOW], kv, ctx, ok, kv_cols)
    kv = jnp.concatenate([kv_ref[0, tokens - 2 * WINDOW :], next_ref[0]], axis=0)
    ok = (pos < 2 * WINDOW) | (sp_ref[0] < n_sp - 1)
    out_ref[WINDOW:] = attend(sink_ref, q_ref[0, tokens - WINDOW :], kv, ctx, ok, kv_cols)


def attend(sink_ref, queries, kv_lat, ctx, inside, kv_cols):
    block = queries.shape[0]
    span = kv_lat.shape[0]
    r = lax.broadcasted_iota(jnp.int32, (block, span), 0)
    c = lax.broadcasted_iota(jnp.int32, (block, span), 1)
    ok = (c >= r) & (c <= r + 2 * WINDOW)
    if inside is not None:
        ok = ok & inside
    bias = jnp.where(ok, 0.0, BIG_NEG)
    local_kv = kv_cols // HEAD_DIM
    per_group = queries.shape[1] // kv_cols
    bias = jnp.concatenate([bias] * per_group, axis=0)
    outs = []
    for n in range(local_kv):
        k_at = slice(n * HEAD_DIM, (n + 1) * HEAD_DIM)
        v_at = slice(kv_cols + n * HEAD_DIM, kv_cols + (n + 1) * HEAD_DIM)
        heads = [n * per_group + g for g in range(per_group)]
        q = jnp.concatenate(
            [queries[:, h * HEAD_DIM : (h + 1) * HEAD_DIM] for h in heads], axis=0
        )
        sink = jnp.concatenate(
            [jnp.full((block, 1), sink_ref[h], jnp.float32) for h in heads], axis=0
        )
        parts = [dot_t(q, kv_lat[:, k_at]) + bias]
        parts += [dot_t(q, t[0, :, k_at]) for t in ctx]
        vals = [kv_lat[:, v_at]] + [t[0, :, v_at] for t in ctx]
        top = sink
        for p in parts:
            top = jnp.maximum(top, jnp.max(p, axis=-1, keepdims=True))
        acc = jnp.zeros((block * per_group, 2 * HEAD_DIM), jnp.float32)
        for p, v in zip(parts, vals):
            e = jnp.exp(p - top).astype(jnp.bfloat16)
            va = jnp.concatenate([v, jnp.ones_like(v)], axis=1)
            acc = acc + jnp.dot(e, va, preferred_element_type=jnp.float32)
        den = acc[:, HEAD_DIM:] + jnp.exp(sink - top)
        o = (acc[:, :HEAD_DIM] / den).astype(jnp.bfloat16)
        outs += [o[g * block : (g + 1) * block] for g in range(per_group)]
    return jnp.concatenate(outs, axis=1)


def out_kernel(*refs, n_src, samples):
    a = refs[: n_src * samples]
    w = refs[n_src * samples : n_src * (samples + 1)]
    at_ref, lat_ref, *mods, out_ref = refs[n_src * (samples + 1) :]
    total = mods[0][at_ref[pl.program_id(0)]]
    for ref in mods[1:]:
        total = total + ref[at_ref[pl.program_id(0)]]
    gate = total[2 * (samples + 1) :]
    rows = lat_ref.shape[1]
    acc = None
    for k in range(n_src):
        lhs = jnp.concatenate([a[s * n_src + k][...] for s in range(samples)], axis=0)
        part = jnp.dot(lhs, w[k][...], preferred_element_type=jnp.float32)
        acc = part if acc is None else acc + part
    for s in range(samples):
        res = lat_ref[s].astype(jnp.float32) + gate[s : s + 1] * acc[s * rows : (s + 1) * rows]
        out_ref[s] = res.astype(jnp.bfloat16)


def full(shape):
    zeros = (0,) * len(shape)
    return pl.BlockSpec(shape, lambda *_: zeros)


def on_device(
    latents,
    context,
    condition,
    cond_context,
    w_shift,
    w_scale,
    w_gate,
    norm_gain,
    w_query,
    w_key,
    w_value,
    sink_logit,
    w_out,
):
    rows, samples, width = latents.shape
    n_tp = lax.axis_size("tp")
    n_sp = lax.axis_size("sp")
    tokens = rows * n_tp
    q_cols = w_query.shape[1]
    kv_cols = w_key.shape[1]
    tp_i = lax.axis_index("tp")
    sp_i = lax.axis_index("sp")
    chips = n_tp // CORES
    order = peers(n_tp)

    smem = pl.BlockSpec(memory_space=pltpu.SMEM)
    vmem = pl.BlockSpec(memory_space=pltpu.VMEM)
    features = w_shift.shape[1]
    n_rows = 3 * samples + 2
    part = pl.pallas_call(
        mod_kernel,
        in_specs=[vmem] * 5,
        out_specs=vmem,
        out_shape=jax.ShapeDtypeStruct((n_rows, features), jnp.float32),
        name="mod_dots",
    )(condition, cond_context[None, :], w_shift, w_scale, w_gate)
    pieces = [
        part if p == (0, 0) else lax.ppermute(part, "tp", peer_perm(n_tp, *p)) for p in order
    ]
    lat_t = jnp.swapaxes(latents, 0, 1)
    lat_own, pieces = lax.optimization_barrier((lat_t, pieces))
    lat_far = across_chips(lat_own, n_tp)
    own_mods = jnp.stack(pieces)
    mods = [own_mods] + [
        lax.ppermute(own_mods, "sp", [(i, (i + k) % n_sp) for i in range(n_sp)])
        for k in range(1, n_sp)
    ]
    at = jnp.stack(
        [
            ((tp_i // CORES - j // CORES) % chips) * CORES + ((tp_i % CORES) ^ (j % CORES))
            for j in range(n_tp)
        ]
    ).astype(jnp.int32)
    gain = norm_gain[None]

    ctx_t = jnp.swapaxes(context, 0, 1)
    ctx_rows = context.shape[0]
    ctx_kv = pl.pallas_call(
        ctx_kernel,
        grid=(samples,),
        in_specs=[
            smem,
            pl.BlockSpec((1, ctx_rows, width), lambda s: (s, 0, 0)),
            full((1, width)),
            full(w_key.shape),
            full(w_value.shape),
        ]
        + [full(own_mods.shape)] * n_sp,
        out_specs=pl.BlockSpec((1, ctx_rows, 2 * kv_cols), lambda s: (s, 0, 0)),
        out_shape=jax.ShapeDtypeStruct((samples, ctx_rows, 2 * kv_cols), jnp.bfloat16),
        name="ctx_proj",
    )(at, ctx_t, gain, w_key, w_value, *mods)
    ctx_blocks = [ctx_kv] + [
        lax.ppermute(ctx_kv, "sp", [(i, (i + k) % n_sp) for i in range(n_sp)])
        for k in range(1, n_sp)
    ]

    offset = sp_i * tokens
    positions = offset + jnp.arange(tokens, dtype=jnp.int32)
    quarter = HEAD_DIM // 4
    lane = jnp.arange(LANES, dtype=jnp.int32)
    inverse = THETA ** (-(lane % quarter).astype(jnp.float32) / quarter)
    is_row = (lane % (2 * quarter) < quarter)[None]
    grid_row = (positions // GRID_W).astype(jnp.float32)[:, None]
    grid_col = (positions % GRID_W).astype(jnp.float32)[:, None]
    angles = jnp.where(is_row, grid_row, grid_col) * inverse[None]
    cosine = jnp.cos(angles)
    sine = jnp.sin(angles) * jnp.where(lane % HEAD_DIM < HEAD_DIM // 2, -1.0, 1.0)[None]

    near = [ctx_blocks[1], ctx_blocks[-1]]
    lat_far, (ctx_blocks[1], ctx_blocks[-1]), cosine, sine = lax.optimization_barrier(
        (lat_far, near, cosine, sine)
    )
    lat_blocks = across_cores(lat_far, n_tp)

    src = jnp.stack(
        [((tp_i // CORES - c) % chips) * CORES + ((tp_i % CORES) ^ e) for c, e in order]
    ).astype(jnp.int32)
    queries, lat_kv = pl.pallas_call(
        functools.partial(proj_kernel, n_src=n_tp, n_mod=n_sp, scale=HEAD_DIM**-0.5),
        in_specs=[smem, smem]
        + [vmem] * 6
        + [pl.BlockSpec(memory_space=pl.ANY)] * n_tp
        + [vmem] * n_sp,
        out_specs=[vmem, vmem],
        out_shape=[
            jax.ShapeDtypeStruct((samples, tokens, q_cols), jnp.bfloat16),
            jax.ShapeDtypeStruct((samples, tokens, 2 * kv_cols), jnp.bfloat16),
        ],
        scratch_shapes=[
            pltpu.VMEM((n_tp, samples, rows, width), jnp.bfloat16),
            pltpu.SemaphoreType.DMA((n_tp,)),
        ],
        name="lat_proj",
    )(
        src,
        at,
        gain,
        cosine,
        sine,
        w_query,
        w_key,
        w_value,
        *lat_blocks,
        *mods,
    )

    ends = n_sp - 1
    before = lax.ppermute(lat_kv[:, tokens - WINDOW :], "sp", [(i, i + 1) for i in range(ends)])
    after = lax.ppermute(lat_kv[:, :WINDOW], "sp", [(i + 1, i) for i in range(ends)])

    w_own, _ = lax.optimization_barrier((w_out, lat_far))
    w_far = across_chips(w_own, n_tp)

    inner = []
    for s in range(samples):
        part_at = functools.partial(lambda s, *_: (s, 0, 0), s)
        own_specs = [
            pl.BlockSpec((1, tokens, q_cols), part_at),
            pl.BlockSpec((1, tokens, 2 * kv_cols), part_at),
        ]
        ctx_specs = [pl.BlockSpec((1, ctx_rows, 2 * kv_cols), part_at)] * n_sp
        inner.append(
            pl.pallas_call(
                functools.partial(interior_kernel, kv_cols=kv_cols),
                grid=(1,),
                in_specs=[smem] + own_specs + ctx_specs,
                out_specs=full((tokens - 2 * WINDOW, q_cols)),
                out_shape=jax.ShapeDtypeStruct((tokens - 2 * WINDOW, q_cols), jnp.bfloat16),
                name="attend_inner",
            )(sink_logit, queries, lat_kv, *ctx_blocks)
        )
    before, after, inner, w_far = lax.optimization_barrier((before, after, inner, w_far))
    w_blocks = across_cores(w_far, n_tp)
    received = []
    for s in range(samples):
        part_at = functools.partial(lambda s, *_: (s, 0, 0), s)
        own_specs = [
            pl.BlockSpec((1, tokens, q_cols), part_at),
            pl.BlockSpec((1, tokens, 2 * kv_cols), part_at),
        ]
        ctx_specs = [pl.BlockSpec((1, ctx_rows, 2 * kv_cols), part_at)] * n_sp
        edges = pl.pallas_call(
            functools.partial(edge_kernel, kv_cols=kv_cols, n_sp=n_sp),
            grid=(1,),
            in_specs=[smem, smem]
            + own_specs
            + [pl.BlockSpec((1, WINDOW, 2 * kv_cols), part_at)] * 2
            + ctx_specs,
            out_specs=full((2 * WINDOW, q_cols)),
            out_shape=jax.ShapeDtypeStruct((2 * WINDOW, q_cols), jnp.bfloat16),
            name="attend_edges",
        )(sp_i.reshape(1), sink_logit, queries, lat_kv, before, after, *ctx_blocks)
        attended = jnp.concatenate([edges[:WINDOW], inner[s], edges[WINDOW:]], axis=0)
        for c, e in order:
            to = ((tp_i // CORES + c) % chips) * CORES + ((tp_i % CORES) ^ e)
            chunk = lax.dynamic_slice_in_dim(attended, to * rows, rows, axis=0)
            if (c, e) != (0, 0):
                chunk = lax.ppermute(chunk, "tp", peer_perm(n_tp, c, e))
            received.append(chunk)

    cols = features
    refined = pl.pallas_call(
        functools.partial(out_kernel, n_src=n_tp, samples=samples),
        grid=(width // cols,),
        in_specs=[full((rows, q_cols))] * (n_tp * samples)
        + [pl.BlockSpec((q_cols, cols), lambda j: (0, j))] * n_tp
        + [
            smem,
            pl.BlockSpec((samples, rows, cols), lambda j: (0, 0, j)),
        ]
        + [full(own_mods.shape)] * n_sp,
        out_specs=pl.BlockSpec((samples, rows, cols), lambda j: (0, 0, j)),
        out_shape=jax.ShapeDtypeStruct((samples, rows, width), jnp.bfloat16),
        name="out_proj",
    )(*received, *w_blocks, at, lat_t, *mods)
    return jnp.swapaxes(refined, 0, 1)


def solution(mesh):
    return jax.shard_map(
        on_device,
        mesh=mesh,
        in_specs=(
            P(("sp", "tp"), "grp", None),
            P("sp", "grp", None),
            P("grp", "sp"),
            P("sp"),
            P("sp", "tp"),
            P("sp", "tp"),
            P("sp", "tp"),
            P(),
            P(None, "tp"),
            P(None, "tp"),
            P(None, "tp"),
            P("tp"),
            P("tp", None),
        ),
        out_specs=P(("sp", "tp"), "grp", None),
        check_vma=False,
    )
```
